32 devices in a mesh: ep: 8 (over z, y), tp: 4 (over x, core).
Axes of the slice: x: 2, y: 2, z: 4, core: 2. Of those that a mesh axis runs over, the one named last changes fastest.
Arguments:
- query_rows: bfloat16 [2048, 2048], P('ep', 'tp'), may hold values from -6 to 6
- key_rows: bfloat16 [2048, 512], P('ep', 'tp'), may hold values from -18 to 18
- value_rows: bfloat16 [2048, 512], P('ep', 'tp'), may hold values from -12 to 12
- key_bias: bfloat16 [2048, 8], P('ep', 'tp'), may hold values from -2 to 13
- head_offset: float32 [32], P('tp'), may hold values from -16 to -3
- out_weight: bfloat16 [2048, 2048], P('tp'), may hold values from -0.125 to 0.125
- expert_input: bfloat16 [4096, 2048], P(('ep', 'tp')), may hold values from -40 to 40
- expert_gain: float32 [2048], replicated, may hold values from 0.1 to 1.9
- routes: int32 [4096, 2], P(('ep', 'tp')), may hold values from 0 to 7, all different within a row; in each aligned block of 128 rows (0 to 127, 128 to 255, ...) at most 48 rows name the same one
- route_weight: float32 [4096, 2], P(('ep', 'tp')), may hold values from 0.5 to 2
- gate_weight: bfloat16 [8, 2048, 3584], P('ep', None, 'tp'), may hold values from -0.125 to 0.125
- up_weight: bfloat16 [8, 2048, 3584], P('ep', None, 'tp'), may hold values from -0.125 to 0.125
- down_weight: bfloat16 [8, 3584, 2048], P('ep', 'tp'), may hold values from -0.09375 to 0.09375
Outputs:
- mixed_a: bfloat16 [2048, 2048], P(('ep', 'tp'))
- mixed_b: bfloat16 [4096, 2048], P(('ep', 'tp'))
The draws below stay inside these ranges and needn't reach their ends.
Inputs may be any that keep to these rules, and one draw needn't show every extreme that they name: `routes`: each row names 2 different experts; in the rows of one device (aligned blocks of 128 rows) no expert is named more than 48 times, and in every draw some device names some expert exactly 48 times.
All inputs are finite; a program needn't handle non-finite values.
Results may differ from the reference program's by a relative error of at most 0.012.
Values may be sent and summed in bfloat16 or wider, within the bound.
A program may use at most 128 MiB of HBM per device.

```python
import math
import jax
import jax.numpy as jnp
import numpy as np
from jax import lax

D = 2048
HEADS = 32
KEY_VALUE_HEADS = 8
HD = 64
FF = 3584
TOPK = 2
TOK_A = 256
TOK_B = 128
SEQUENCE_LEN_A = 2048
TOKENS_B = 4096
EXPERTS = 8
CAP = 48
N_EP = 8
N_TP = 4


def draw_head_offset(key, part):
    first_key, second_key, key_third_part = jax.random.split(jax.random.fold_in(key, 17), 3)
    picks = jax.random.randint(first_key, (HEADS,), 0, 8)
    slow_heads = picks < 4
    slow_value = -4.5 - math.log(SEQUENCE_LEN_A) + jax.random.uniform(second_key, (HEADS,), jnp.float32, -0.5, 0.5)
    fast_value = jax.random.uniform(key_third_part, (HEADS,), jnp.float32, -5.0, -3.0)
    return jnp.where(slow_heads, slow_value, fast_value).astype(jnp.float32)


def draw_key_bias(key, part):
    first_key, second_key, key_third_part = jax.random.split(jax.random.fold_in(key, 23), 3)
    spread = 0.8
    block_count = SEQUENCE_LEN_A // TOK_A
    factors = jax.random.uniform(first_key, (block_count, 1, KEY_VALUE_HEADS), jnp.float32, -spread, spread)
    factors = jnp.broadcast_to(factors, (block_count, TOK_A, KEY_VALUE_HEADS)).reshape(SEQUENCE_LEN_A, KEY_VALUE_HEADS)
    noise = 0.3 * jax.random.normal(second_key, (SEQUENCE_LEN_A, KEY_VALUE_HEADS), jnp.float32)
    start_offset = jnp.clip(factors + noise, -1.5, 1.5)
    group_position = jax.random.randint(key_third_part, (2, KEY_VALUE_HEADS), 0, SEQUENCE_LEN_A)
    token_group = jnp.any(jnp.arange(SEQUENCE_LEN_A)[:, None, None] == group_position[None, :, :], axis=1)
    return (start_offset + 11.0 * token_group.astype(jnp.float32)).astype(jnp.bfloat16)


def draw_expert_input(key, part):
    first_key, second_key = jax.random.split(jax.random.fold_in(key, 31), 2)
    scales = jnp.exp(jax.random.uniform(first_key, (TOKENS_B, 1), jnp.float32, 0.0, math.log(10.0)))
    values = jnp.clip(jax.random.normal(second_key, (TOKENS_B, D), jnp.float32), -4.0, 4.0)
    return (values * scales).astype(jnp.bfloat16)


def level_of(stream_key, dims, shards, low, high):
    level, own = 1.0, jax.random.fold_in(stream_key, 6)
    for position, blocks in shards:
        heights = jnp.exp(jax.random.uniform(jax.random.fold_in(own, position), (blocks,), jnp.float32, low / len(shards), high / len(shards)))
        level = level * jnp.repeat(heights, dims[position] // blocks).reshape([-1 if axis == position else 1 for axis in range(len(dims))])
    return level


def shared_out(own_key, own, number, rows, number_of, top, reach, slope):
    sequence = jax.random.permutation(own_key, number_of)
    heavy_load, usual = portions_of(number_of, rows * top, reach, slope, True), portions_of(number_of, rows * top, reach, slope, False)
    places = jnp.arange(number_of)

    def named(tallies, offset_by):
        used = int((tallies > 0).sum())
        fixed = max(1, used // 4)
        moved = fixed + (places - fixed + offset_by * (used - fixed)) % max(1, number_of - fixed)
        return jnp.zeros((number_of,), jnp.int32).at[sequence[jnp.where(places < fixed, places, moved)]].set(jnp.asarray(tallies, jnp.int32))

    tallies = jnp.where(number % 4 == 0, named(heavy_load, number // 4), named(usual, number - number // 4 - 1))
    mixed = jax.random.permutation(jax.random.fold_in(own, 3), number_of)
    source_of, taker = mixed[0:number_of // 2 * 2:2], mixed[1:number_of // 2 * 2:2]
    slack = jnp.minimum(tallies[source_of] - 1, reach - tallies[taker]) // 2
    slack = jnp.where((source_of == sequence[0]) | (taker == sequence[0]) | (tallies[taker] == 0), 0, jnp.maximum(slack, 0))
    moved = jax.random.randint(jax.random.fold_in(own, 4), (number_of // 2,), 0, 1 << 20) % (slack + 1)
    tallies = tallies.at[source_of].add(-moved).at[taker].add(moved)
    items = jnp.searchsorted(jnp.cumsum(tallies), jnp.arange(rows * top), side="right").astype(jnp.int32)
    listing = items.reshape(top, rows).T
    listing = listing[jax.random.permutation(jax.random.fold_in(own, 1), rows)]
    offset_by = jax.random.randint(jax.random.fold_in(own, 2), (rows, 1), 0, top)
    return jnp.take_along_axis(listing, (jnp.arange(top)[None, :] + offset_by) % top, axis=1)


def portions_of(number_of, total, most, slope, full):
    weights = [(1 << 20) // math.isqrt(standing ** slope) + 1 for standing in range(1, number_of + 1)]
    largest = most if full else min(most, max(-(-total // number_of), total * weights[0] // sum(weights)))
    least = 1 if total - largest >= number_of - 1 else 0
    given, surplus = [largest] + [least] * (number_of - 1), total - largest - least * (number_of - 1)
    while surplus > 0:
        free = [i for i in range(1, number_of) if given[i] < largest] or [i for i in range(1, number_of) if given[i] < most]
        pool, remaining = sum([weights[i] for i in free]), surplus
        for i in free:
            addition = min(most - given[i], max(1, remaining * weights[i] // pool), surplus)
            given[i] = given[i] + addition
            surplus = surplus - addition
    return np.array(given)


def normal_values(own_key, extent, scale, reach, cuts=(), kind=jnp.bfloat16):
    entries = jax.random.normal(own_key, extent, jnp.float32) * scale
    if len(cuts) > 0:
        entries = level_of(own_key, extent, cuts, -0.22, 0.18) * entries
    return jnp.clip(entries, min=-reach, max=reach).astype(kind)


def setup_inputs(seed: int = 0) -> dict:
    seeds = jax.random.split(jax.random.key(seed), 14)
    query_rows = normal_values(seeds[0], (SEQUENCE_LEN_A, HEADS * HD), 1.0, 6.0, ((0, 8), (1, 4)))
    key_rows = normal_values(seeds[1], (SEQUENCE_LEN_A, KEY_VALUE_HEADS * HD), 3.0, 18.0, ((0, 8), (1, 4)))
    value_rows = normal_values(seeds[2], (SEQUENCE_LEN_A, KEY_VALUE_HEADS * HD), 2.0, 12.0, ((0, 8), (1, 4)))
    key_bias = draw_key_bias(jax.random.fold_in(seeds[13], 71), 0)
    head_offset = draw_head_offset(jax.random.fold_in(seeds[13], 71), 0)
    out_weight = normal_values(seeds[5], (HEADS * HD, D), (HEADS * HD) ** -0.5, 0.125, ((0, 4),))
    expert_input = draw_expert_input(jax.random.fold_in(seeds[13], 71), 0)
    expert_gain = jnp.clip(1.0 + 0.18 * jax.random.normal(seeds[7], (D,), jnp.float32), 0.1, 1.9)
    routes_keys = jax.random.split(jax.random.fold_in(seeds[8], 1), TOKENS_B // TOK_B)
    routes_turns = jax.random.permutation(jax.random.fold_in(seeds[8], 3), TOKENS_B // TOK_B)
    routes = jax.vmap(lambda own, number: shared_out(jax.random.fold_in(seeds[8], 2), own, number, TOK_B, EXPERTS, TOPK, CAP, 1))(routes_keys, routes_turns).reshape((TOKENS_B, TOPK))
    route_weight = jnp.clip(0.5 + 1.5 * jax.random.uniform(seeds[9], (TOKENS_B, TOPK), jnp.float32) ** level_of(seeds[9], (TOKENS_B, TOPK), ((0, 32),), -0.2, 0.2), 0.5, 2.0)
    gate_weight = normal_values(seeds[10], (EXPERTS, D, FF), D ** -0.5, 0.125, ((0, 8), (2, 4)))
    up_weight = normal_values(seeds[11], (EXPERTS, D, FF), D ** -0.5, 0.125, ((0, 8), (2, 4)))
    down_weight = normal_values(seeds[12], (EXPERTS, FF, D), FF ** -0.5, 0.09375, ((0, 8), (1, 4)))
    return {"query_rows": query_rows, "key_rows": key_rows, "value_rows": value_rows, "key_bias": key_bias, "head_offset": head_offset, "out_weight": out_weight, "expert_input": expert_input, "expert_gain": expert_gain, "routes": routes, "route_weight": route_weight, "gate_weight": gate_weight, "up_weight": up_weight, "down_weight": down_weight}


EPSILON = 1e-06

def rms_normed(rows, gain):
    values = rows.astype(jnp.float32)
    scaled = values * lax.rsqrt(lax.optimization_barrier(jnp.mean(values * values, axis=-1, keepdims=True)) + EPSILON)
    return (scaled * gain).astype(jnp.bfloat16)

def stick_heads(query_rows, key_rows, value_rows, key_bias, head_offset):
    group_size = HEADS // KEY_VALUE_HEADS
    queries4 = query_rows.astype(jnp.float32).reshape(SEQUENCE_LEN_A, KEY_VALUE_HEADS, group_size, HD)
    key_heads = key_rows.astype(jnp.float32).reshape(SEQUENCE_LEN_A, KEY_VALUE_HEADS, HD)
    value_heads = value_rows.astype(jnp.float32).reshape(SEQUENCE_LEN_A, KEY_VALUE_HEADS, HD)
    offsets = head_offset.reshape(KEY_VALUE_HEADS, group_size)
    bias_rows = jnp.transpose(key_bias.astype(jnp.float32))
    block_rows = math.gcd(TOK_A, 128)
    key_pos = jnp.arange(SEQUENCE_LEN_A, dtype=jnp.int32)

    def one_block(block_turn):
        first_row = (block_turn * block_rows).astype(jnp.int32)
        query_block = lax.dynamic_slice_in_dim(queries4, first_row, block_rows, 0)
        scores = jnp.einsum('qgjd,kgd->gjqk', query_block, key_heads) * (1.0 / math.sqrt(HD))
        scores = scores + offsets[:, :, None, None] + bias_rows[:, None, None, :]
        query_pos = first_row + jnp.arange(block_rows, dtype=jnp.int32)
        keep_mask = key_pos[None, :] < query_pos[:, None]
        log_stay = jnp.where(keep_mask, jax.nn.log_sigmoid(-scores), 0.0)
        after_sum = lax.cumsum(log_stay, axis=3, reverse=True) - log_stay
        weights = jnp.where(keep_mask, jnp.exp(jax.nn.log_sigmoid(scores) + after_sum), 0.0).astype(jnp.bfloat16)
        weights = lax.optimization_barrier(weights).astype(jnp.float32)
        return jnp.einsum('gjqk,kgd->qgjd', weights, value_heads).reshape(block_rows, HEADS * HD)
    blocks = lax.map(one_block, jnp.arange(SEQUENCE_LEN_A // block_rows, dtype=jnp.int32))
    return blocks.reshape(SEQUENCE_LEN_A, HEADS * HD).astype(jnp.bfloat16)

def reference(query_rows, key_rows, value_rows, key_bias, head_offset, out_weight, expert_input, expert_gain, routes, route_weight, gate_weight, up_weight, down_weight):
    heads_out = stick_heads(query_rows, key_rows, value_rows, key_bias, head_offset)
    col_part = HEADS * HD // N_TP
    total_sum = jnp.zeros((SEQUENCE_LEN_A, D), jnp.float32)
    for tp_part in range(N_TP):
        lower = tp_part * col_part
        partial_value = jnp.dot(heads_out[:, lower:lower + col_part], out_weight[lower:lower + col_part], preferred_element_type=jnp.float32).astype(jnp.bfloat16)
        total_sum = total_sum + lax.optimization_barrier(partial_value).astype(jnp.float32)
    mixed_a = total_sum.astype(jnp.bfloat16)
    normed = rms_normed(expert_input, expert_gain)
    flat_route = routes.reshape(-1)
    flat_token = (jnp.arange(TOKENS_B * TOPK, dtype=jnp.int32) // TOPK).astype(jnp.int32)
    flattened_weight = route_weight.reshape(-1)
    row_limit = N_EP * N_TP * CAP
    hidden_part = FF // N_TP

    def one_expert(expert_id):
        order_rows = jnp.argsort((flat_route != expert_id).astype(jnp.int32), stable=True)[:row_limit].astype(jnp.int32)
        live = flat_route[order_rows] == expert_id
        inputs = normed[flat_token[order_rows]]
        gate_act = jnp.dot(inputs, gate_weight[expert_id], preferred_element_type=jnp.float32)
        up_act = jnp.dot(inputs, up_weight[expert_id], preferred_element_type=jnp.float32)
        hidden = (jax.nn.silu(gate_act) * up_act).astype(jnp.bfloat16)
        down_rows = down_weight[expert_id]
        expert_sum = jnp.zeros((row_limit, D), jnp.float32)
        for tp_part in range(N_TP):
            lower = tp_part * hidden_part
            partial_value = jnp.dot(hidden[:, lower:lower + hidden_part], down_rows[lower:lower + hidden_part], preferred_element_type=jnp.float32).astype(jnp.bfloat16)
            expert_sum = expert_sum + lax.optimization_barrier(partial_value).astype(jnp.float32)
        result = lax.optimization_barrier(expert_sum.astype(jnp.bfloat16)).astype(jnp.float32)
        scaled = result * jnp.where(live, flattened_weight[order_rows], 0.0)[:, None]
        return (order_rows, scaled)
    orders, results = lax.map(one_expert, jnp.arange(EXPERTS, dtype=jnp.int32))
    combined = jnp.zeros((TOKENS_B, D), jnp.float32).at[flat_token[orders.reshape(-1)]].add(results.reshape(-1, D))
    mixed_b = combined.astype(jnp.bfloat16)
    return (mixed_a, mixed_b)
```

```python
import functools
import math

import jax
import jax.numpy as jnp
from jax import lax
from jax.experimental import pallas as pl
from jax.experimental.pallas import tpu as pltpu
from jax.sharding import PartitionSpec as P

HD = 64


EPSILON = 1e-06


def rms_normed(rows, gain):
    values = rows.astype(jnp.float32)
    scaled = values * lax.rsqrt(jnp.mean(values * values, axis=-1, keepdims=True) + EPSILON)
    return (scaled * gain).astype(jnp.bfloat16)


def stick_kernel(q_ref, kv_ref, tri_ref, out_ref, acc_ref, carry_ref, *, kv_local, group_size):
    block = out_ref.shape[0]
    wide = 2 * HD
    me = lax.axis_index("ep")
    acc_ref[...] = jnp.zeros_like(acc_ref)
    carry_ref[...] = jnp.zeros_like(carry_ref)
    value_width = kv_local * HD

    def tile(index, keep):
        first = pl.multiple_of(index * block, block)
        values = kv_ref[pl.ds(first, block), kv_local * wide : kv_local * wide + value_width]
        for kv in range(kv_local):
            keys = kv_ref[pl.ds(first, block), kv * wide : (kv + 1) * wide]
            for head in range(kv * group_size, (kv + 1) * group_size):
                rows = slice(head * block, (head + 1) * block)
                scores = lax.dot_general(
                    q_ref[rows, :], keys, (((1,), (1,)), ((), ())),
                    preferred_element_type=jnp.float32,
                )
                leave = jnp.maximum(scores, 0.0) + jnp.log(1.0 + jnp.exp(-jnp.abs(scores)))
                log_take = scores - leave
                if keep is not None:
                    leave = jnp.where(keep, leave, 0.0)
                high = leave.astype(jnp.bfloat16)
                low = (leave - high.astype(jnp.float32)).astype(jnp.bfloat16)
                after = jnp.dot(high, tri_ref[...], preferred_element_type=jnp.float32) + jnp.dot(
                    low, tri_ref[...], preferred_element_type=jnp.float32
                )
                carry = carry_ref[rows, :]
                weights = jnp.exp(log_take - after - carry)
                if keep is not None:
                    weights = jnp.where(keep, weights, 0.0)
                acc_ref[rows, :] += jnp.dot(
                    weights.astype(jnp.bfloat16), values, preferred_element_type=jnp.float32
                )
                carry_ref[rows, :] = carry + jnp.broadcast_to(
                    after[:, :1] + leave[:, :1], carry.shape
                )

    query_index = lax.broadcasted_iota(jnp.int32, (block, block), 0)
    key_index = lax.broadcasted_iota(jnp.int32, (block, block), 1)
    tile(me, key_index < query_index)

    def earlier(step, unused):
        tile(me - 1 - step, None)
        return unused

    lax.fori_loop(0, me, earlier, 0)
    for head in range(0, kv_local * group_size):
        kv = head // group_size
        rows = slice(head * block, (head + 1) * block)
        out_ref[:, head * HD : (head + 1) * HD] = acc_ref[rows, kv * HD : (kv + 1) * HD].astype(
            jnp.bfloat16
        )


def stick_heads(query_rows, key_rows, value_rows, key_bias, head_offset):
    block = query_rows.shape[0]
    kv_local = key_rows.shape[1] // HD
    heads = query_rows.shape[1] // HD
    group_size = heads // kv_local
    wide = 2 * HD
    one = jnp.ones((block, kv_local, 3), jnp.bfloat16)
    key_wide = jnp.concatenate(
        [
            key_rows.reshape(block, kv_local, HD),
            key_bias[:, :, None],
            one,
            jnp.zeros((block, kv_local, wide - HD - 4), jnp.bfloat16),
        ],
        axis=2,
    ).reshape(block, kv_local * wide)
    packed = jnp.concatenate([key_wide, value_rows], axis=1)
    all_packed = lax.all_gather(packed, "ep", axis=0, tiled=True)
    first = lax.reduce_precision(head_offset, 8, 7)
    second = lax.reduce_precision(head_offset - first, 8, 7)
    third = head_offset - first - second
    terms = jnp.stack([jnp.ones_like(first), first, second, third], axis=1).astype(jnp.bfloat16)
    queries = jnp.transpose(query_rows.reshape(block, heads, HD), (1, 0, 2)) * jnp.bfloat16(
        1.0 / math.sqrt(HD)
    )
    query_wide = jnp.concatenate(
        [
            queries,
            jnp.broadcast_to(terms[:, None, :], (heads, block, 4)),
            jnp.zeros((heads, block, wide - HD - 4), jnp.bfloat16),
        ],
        axis=2,
    ).reshape(heads * block, wide)
    place = jnp.arange(block)
    tri = (place[:, None] > place[None, :]).astype(jnp.bfloat16)
    span = all_packed.shape[0]
    cells = heads * block * span
    return pl.pallas_call(
        functools.partial(stick_kernel, kv_local=kv_local, group_size=group_size),
        out_shape=jax.ShapeDtypeStruct((block, heads * HD), jnp.bfloat16),
        in_specs=[pl.BlockSpec(memory_space=pltpu.VMEM)] * 3,
        out_specs=pl.BlockSpec(memory_space=pltpu.VMEM),
        scratch_shapes=[
            pltpu.VMEM((heads * block, kv_local * HD), jnp.float32),
            pltpu.VMEM((heads * block, 1), jnp.float32),
        ],
        compiler_params=pltpu.CompilerParams(vmem_limit_bytes=24 * 1024 * 1024),
        cost_estimate=pl.CostEstimate(
            flops=cells * 1000, bytes_accessed=span * 768, transcendentals=cells * 3
        ),
        name="stick",
    )(query_wide, all_packed, tri)


def body(
    query_rows,
    key_rows,
    value_rows,
    key_bias,
    head_offset,
    out_weight,
    expert_input,
    expert_gain,
    routes,
    route_weight,
    gate_weight,
    up_weight,
    down_weight,
):
    heads_out = stick_heads(query_rows, key_rows, value_rows, key_bias, head_offset)
    mixed_a = lax.psum_scatter(
        jnp.dot(heads_out, out_weight, preferred_element_type=jnp.float32).astype(jnp.bfloat16),
        "tp",
        scatter_dimension=0,
        tiled=True,
    )
    normed = rms_normed(expert_input, expert_gain)
    tok_count = normed.shape[0]
    top_count = routes.shape[1]
    model_width = normed.shape[1]
    expert_count = lax.axis_size("ep")
    capacity = max(2, 3 * tok_count * top_count // (2 * expert_count))
    flat_route = routes.reshape(-1)
    one_hot = (flat_route[:, None] == jnp.arange(expert_count)[None, :]).astype(jnp.int32)
    before = jnp.cumsum(one_hot, axis=0) - one_hot
    slot_index = (flat_route * capacity + jnp.sum(before * one_hot, axis=1)).reshape(
        tok_count, top_count
    )
    slot_ids = jnp.arange(expert_count * capacity)
    dispatch = jnp.sum(
        (slot_index[None, :, :] == slot_ids[:, None, None]).astype(jnp.int32), axis=2
    ).astype(jnp.bfloat16)
    outgoing = (
        jnp.dot(dispatch, normed, preferred_element_type=jnp.float32)
        .astype(jnp.bfloat16)
        .reshape(expert_count, capacity, model_width)
    )
    source_rows = expert_count * capacity
    arrived = lax.all_to_all(outgoing, "ep", split_axis=0, concat_axis=0, tiled=True)
    row_piece = lax.all_gather(arrived.reshape(source_rows, model_width), "tp", axis=0, tiled=True)
    gate_act = jnp.dot(row_piece, gate_weight[0], preferred_element_type=jnp.float32)
    up_act = jnp.dot(row_piece, up_weight[0], preferred_element_type=jnp.float32)
    hidden_all = (jax.nn.silu(gate_act) * up_act).astype(jnp.bfloat16)
    expert_result = lax.psum_scatter(
        jnp.dot(hidden_all, down_weight[0], preferred_element_type=jnp.float32).astype(
            jnp.bfloat16
        ),
        "tp",
        scatter_dimension=0,
        tiled=True,
    )
    returned = lax.all_to_all(
        expert_result.reshape(expert_count, capacity, model_width),
        "ep",
        split_axis=0,
        concat_axis=0,
        tiled=True,
    )
    picked_rows = returned.reshape(-1, model_width)[slot_index.reshape(-1)].reshape(
        tok_count, top_count, model_width
    )
    mixed_b = jnp.sum(picked_rows.astype(jnp.float32) * route_weight[:, :, None], axis=1).astype(
        jnp.bfloat16
    )
    return (mixed_a, mixed_b)


def solution(mesh):
    return jax.shard_map(
        body,
        mesh=mesh,
        in_specs=(
            P("ep", "tp"),
            P("ep", "tp"),
            P("ep", "tp"),
            P("ep", "tp"),
            P("tp"),
            P("tp", None),
            P(("ep", "tp"), None),
            P(),
            P(("ep", "tp"), None),
            P(("ep", "tp"), None),
            P("ep", None, "tp"),
            P("ep", None, "tp"),
            P("ep", "tp", None),
        ),
        out_specs=(P(("ep", "tp"), None), P(("ep", "tp"), None)),
        check_vma=False,
    )
```

```python
import functools
import math

import jax
import jax.numpy as jnp
from jax import lax
from jax.experimental import pallas as pl
from jax.experimental.pallas import tpu as pltpu
from jax.sharding import PartitionSpec as P

HD = 64


EPSILON = 1e-06
CHUNKS = 2


def rms_normed(rows, gain):
    values = rows.astype(jnp.float32)
    scaled = values * lax.rsqrt(jnp.mean(values * values, axis=-1, keepdims=True) + EPSILON)
    return (scaled * gain).astype(jnp.bfloat16)


def stick_kernel(q_ref, kv_ref, tri_ref, out_ref, acc_ref, carry_ref, *, kv_local, group_size):
    block = out_ref.shape[0]
    wide = 2 * HD
    me = lax.axis_index("ep")
    acc_ref[...] = jnp.zeros_like(acc_ref)
    carry_ref[...] = jnp.zeros_like(carry_ref)
    value_width = kv_local * HD

    def tile(index, keep):
        first = pl.multiple_of(index * block, block)
        values = kv_ref[pl.ds(first, block), kv_local * wide : kv_local * wide + value_width]
        for kv in range(kv_local):
            keys = kv_ref[pl.ds(first, block), kv * wide : (kv + 1) * wide]
            for head in range(kv * group_size, (kv + 1) * group_size):
                rows = slice(head * block, (head + 1) * block)
                scores = lax.dot_general(
                    q_ref[rows, :], keys, (((1,), (1,)), ((), ())),
                    preferred_element_type=jnp.float32,
                )
                leave = jnp.maximum(scores, 0.0) + jnp.log(1.0 + jnp.exp(-jnp.abs(scores)))
                log_take = scores - leave
                if keep is not None:
                    leave = jnp.where(keep, leave, 0.0)
                high = leave.astype(jnp.bfloat16)
                low = (leave - high.astype(jnp.float32)).astype(jnp.bfloat16)
                after = jnp.dot(high, tri_ref[...], preferred_element_type=jnp.float32) + jnp.dot(
                    low, tri_ref[...], preferred_element_type=jnp.float32
                )
                carry = carry_ref[rows, :]
                weights = jnp.exp(log_take - after - carry)
                if keep is not None:
                    weights = jnp.where(keep, weights, 0.0)
                acc_ref[rows, :] += jnp.dot(
                    weights.astype(jnp.bfloat16), values, preferred_element_type=jnp.float32
                )
                carry_ref[rows, :] = carry + jnp.broadcast_to(
                    after[:, :1] + leave[:, :1], carry.shape
                )

    query_index = lax.broadcasted_iota(jnp.int32, (block, block), 0)
    key_index = lax.broadcasted_iota(jnp.int32, (block, block), 1)
    tile(me, key_index < query_index)

    def earlier(step, unused):
        tile(me - 1 - step, None)
        return unused

    lax.fori_loop(0, me, earlier, 0)
    for head in range(0, kv_local * group_size):
        kv = head // group_size
        rows = slice(head * block, (head + 1) * block)
        out_ref[:, head * HD : (head + 1) * HD] = acc_ref[rows, kv * HD : (kv + 1) * HD].astype(
            jnp.bfloat16
        )


def gather_keys(key_rows, value_rows, key_bias):
    block = key_rows.shape[0]
    kv_local = key_rows.shape[1] // HD
    wide = 2 * HD
    one = jnp.ones((block, kv_local, 3), jnp.bfloat16)
    key_wide = jnp.concatenate(
        [
            key_rows.reshape(block, kv_local, HD),
            key_bias[:, :, None],
            one,
            jnp.zeros((block, kv_local, wide - HD - 4), jnp.bfloat16),
        ],
        axis=2,
    ).reshape(block, kv_local * wide)
    packed = jnp.concatenate([key_wide, value_rows], axis=1)
    return lax.all_gather(packed, "ep", axis=0, tiled=True)


def stick_heads(query_rows, all_packed, head_offset, kv_local):
    block = query_rows.shape[0]
    heads = query_rows.shape[1] // HD
    group_size = heads // kv_local
    wide = 2 * HD
    first = lax.reduce_precision(head_offset, 8, 7)
    second = lax.reduce_precision(head_offset - first, 8, 7)
    third = head_offset - first - second
    terms = jnp.stack([jnp.ones_like(first), first, second, third], axis=1).astype(jnp.bfloat16)
    queries = jnp.transpose(query_rows.reshape(block, heads, HD), (1, 0, 2)) * jnp.bfloat16(
        1.0 / math.sqrt(HD)
    )
    query_wide = jnp.concatenate(
        [
            queries,
            jnp.broadcast_to(terms[:, None, :], (heads, block, 4)),
            jnp.zeros((heads, block, wide - HD - 4), jnp.bfloat16),
        ],
        axis=2,
    ).reshape(heads * block, wide)
    place = jnp.arange(block)
    tri = (place[:, None] > place[None, :]).astype(jnp.bfloat16)
    span = all_packed.shape[0]
    cells = heads * block * span
    return pl.pallas_call(
        functools.partial(stick_kernel, kv_local=kv_local, group_size=group_size),
        out_shape=jax.ShapeDtypeStruct((block, heads * HD), jnp.bfloat16),
        in_specs=[pl.BlockSpec(memory_space=pltpu.VMEM)] * 3,
        out_specs=pl.BlockSpec(memory_space=pltpu.VMEM),
        scratch_shapes=[
            pltpu.VMEM((heads * block, kv_local * HD), jnp.float32),
            pltpu.VMEM((heads * block, 1), jnp.float32),
        ],
        compiler_params=pltpu.CompilerParams(vmem_limit_bytes=24 * 1024 * 1024),
        cost_estimate=pl.CostEstimate(
            flops=cells * 1000, bytes_accessed=span * 768, transcendentals=cells * 3
        ),
        name="stick",
    )(query_wide, all_packed, tri)


def body(
    query_rows,
    key_rows,
    value_rows,
    key_bias,
    head_offset,
    out_weight,
    expert_input,
    expert_gain,
    routes,
    route_weight,
    gate_weight,
    up_weight,
    down_weight,
):
    kv_local = key_rows.shape[1] // HD
    all_packed = gather_keys(key_rows, value_rows, key_bias)
    normed = rms_normed(expert_input, expert_gain)
    tok_count = normed.shape[0]
    top_count = routes.shape[1]
    model_width = normed.shape[1]
    expert_count = lax.axis_size("ep")
    capacity = max(2, 3 * tok_count * top_count // (2 * expert_count))
    chunks = CHUNKS if capacity % CHUNKS == 0 else 1
    piece = capacity // chunks
    flat_route = routes.reshape(-1)
    one_hot = (flat_route[:, None] == jnp.arange(expert_count)[None, :]).astype(jnp.int32)
    before = jnp.cumsum(one_hot, axis=0) - one_hot
    slot_index = (flat_route * capacity + jnp.sum(before * one_hot, axis=1)).reshape(
        tok_count, top_count
    )
    chunk_rows = expert_count * piece
    hits, arrived = [], []
    for chunk in range(chunks):
        slot_ids = (
            jnp.arange(expert_count)[:, None] * capacity + chunk * piece + jnp.arange(piece)[None, :]
        ).reshape(-1)
        hit = slot_index[None, :, :] == slot_ids[:, None, None]
        hits.append(hit)
        outgoing = jnp.dot(
            jnp.any(hit, axis=2).astype(jnp.bfloat16), normed, preferred_element_type=jnp.float32
        ).astype(jnp.bfloat16)
        outgoing = outgoing.reshape(expert_count, piece, model_width)
        if chunk > 0:
            outgoing, arrived[-1] = lax.optimization_barrier((outgoing, arrived[-1]))
        arrived.append(lax.all_to_all(outgoing, "ep", split_axis=0, concat_axis=0, tiled=True))
    arrived[0], all_packed = lax.optimization_barrier((arrived[0], all_packed))
    results = []
    for chunk in range(chunks):
        row_piece = lax.all_gather(
            arrived[chunk].reshape(chunk_rows, model_width), "tp", axis=0, tiled=True
        )
        gate_act = jnp.dot(row_piece, gate_weight[0], preferred_element_type=jnp.float32)
        up_act = jnp.dot(row_piece, up_weight[0], preferred_element_type=jnp.float32)
        hidden_all = (jax.nn.silu(gate_act) * up_act).astype(jnp.bfloat16)
        partial_sum = jnp.dot(
            hidden_all, down_weight[0], preferred_element_type=jnp.float32
        ).astype(jnp.bfloat16)
        if chunk == chunks - 1:
            partial_sum, query_rows = lax.optimization_barrier((partial_sum, query_rows))
        results.append(
            lax.psum_scatter(partial_sum, "tp", scatter_dimension=0, tiled=True)
        )
    heads_out = stick_heads(query_rows, all_packed, head_offset, kv_local)
    results[0], heads_out = lax.optimization_barrier((results[0], heads_out))
    mixed_a = lax.psum_scatter(
        jnp.dot(heads_out, out_weight, preferred_element_type=jnp.float32).astype(jnp.bfloat16),
        "tp",
        scatter_dimension=0,
        tiled=True,
    )
    total = jnp.zeros((tok_count, model_width), jnp.float32)
    for chunk in range(chunks):
        returned = lax.all_to_all(
            results[chunk].reshape(expert_count, piece, model_width),
            "ep",
            split_axis=0,
            concat_axis=0,
            tiled=True,
        ).reshape(chunk_rows, model_width)
        share = jnp.sum(jnp.where(hits[chunk], route_weight[None, :, :], 0.0), axis=2).T
        for _ in range(3):
            part = lax.reduce_precision(share, 8, 7)
            share = share - part
            total = total + jnp.dot(
                part.astype(jnp.bfloat16), returned, preferred_element_type=jnp.float32
            )
    return (mixed_a, total.astype(jnp.bfloat16))


def solution(mesh):
    return jax.shard_map(
        body,
        mesh=mesh,
        in_specs=(
            P("ep", "tp"),
            P("ep", "tp"),
            P("ep", "tp"),
            P("ep", "tp"),
            P("tp"),
            P("tp", None),
            P(("ep", "tp"), None),
            P(),
            P(("ep", "tp"), None),
            P(("ep", "tp"), None),
            P("ep", None, "tp"),
            P("ep", None, "tp"),
            P("ep", "tp", None),
        ),
        out_specs=(P(("ep", "tp"), None), P(("ep", "tp"), None)),
        check_vma=False,
    )
```
